512 devices in a mesh: grp: 2 (over y), ra: 16 (over z), cb: 16 (over x, core).
Axes of the slice: x: 8, y: 2, z: 16, core: 2. Of those that a mesh axis runs over, the one named last changes fastest.
The devices are a block of a 8x16x16 slice.
Arguments:
- residual: bfloat16 [512, 4096], P('grp', 'ra'), parts along dimension 0, may hold values from -6 to 6
- gain_first: bfloat16 [4096], P('ra'), may hold values from 0.099609375 to 1.8984375
- gate_first: bfloat16 [4096, 11264], P('ra', 'cb'), may hold values from -0.09375 to 0.09375
- up_first: bfloat16 [4096, 11264], P('ra', 'cb'), may hold values from -0.09375 to 0.09375
- down_first: bfloat16 [11264, 4096], P('cb', 'ra'), may hold values from -0.078125 to 0.078125
- gain_second: bfloat16 [4096], P('ra'), may hold values from 0.099609375 to 1.8984375
- gate_second: bfloat16 [4096, 11264], P('ra', 'cb'), may hold values from -0.09375 to 0.09375
- up_second: bfloat16 [4096, 11264], P('ra', 'cb'), may hold values from -0.09375 to 0.09375
- down_second: bfloat16 [11264, 4096], P('cb', 'ra'), may hold values from -0.078125 to 0.078125
Outputs:
- updated: bfloat16 [512, 4096], P('grp', 'ra'), parts along dimension 0
The draws below stay inside these ranges and needn't reach their ends.
There are 2 independent parts, one for each index of `grp`. The reference program is written for one: setup_inputs(seed, part) draws one part's arguments, and reference() takes and returns one part's arrays. A program takes and returns all parts, laid end to end along the dimension named above; an argument that names none is the same for every part. Nothing has to cross between parts.
All inputs are finite; a program needn't handle non-finite values.
Results may differ from the reference program's by a relative error of at most 0.0071.
Values may be sent and summed in bfloat16 or wider, within the bound.
No kernel may reach another device: no remote copies, remote signals or barrier semaphores. Data moves between devices by JAX's collectives and lax.ppermute only.
A program may use at most 64 MiB of HBM per device.

```python
import jax
import jax.numpy as jnp
from jax import lax

D = 4096
FF = 11264
TOK = 256


def draw_residual(key, part):
    first, second, third = jax.random.split(jax.random.fold_in(key, 11), 3)
    rows = jnp.exp(jax.random.uniform(first, (TOK, 1), jnp.float32, jnp.log(0.25), jnp.log(2.5)))
    ramp = jnp.exp(jnp.linspace(jnp.log(0.5), jnp.log(2.0), D)).astype(jnp.float32)
    columns = ramp[None, :] * jnp.exp(jax.random.uniform(third, (1, D), jnp.float32, -0.3, 0.3))
    base = jnp.clip(jax.random.normal(second, (TOK, D), jnp.float32), -4.0, 4.0)
    return jnp.clip(0.4 * rows * columns * base, -6.0, 6.0).astype(jnp.bfloat16)


def spiked(values, stream_key, source, target, blocks, factor):
    def block_of(position):
        return (jnp.arange(values.shape[position]) // (values.shape[position] // blocks)).reshape((-1,) + (1,) * (values.ndim - 1 - position))

    near = jax.random.permutation(stream_key, blocks)[block_of(target)]
    far = (block_of(target) + blocks // 2) % blocks
    return jnp.where((block_of(source) == near) | (block_of(source) == far), factor * values, values)


def level_of(own_key, extent, cuts, smallest, high):
    def one(position, shards_of):
        heights = jax.random.uniform(jax.random.fold_in(jax.random.fold_in(own_key, 6), position), (shards_of,), jnp.float32, smallest / len(cuts), high / len(cuts))
        return jnp.repeat(jnp.exp(heights), extent[position] // shards_of).reshape((-1,) + (1,) * (len(extent) - position - 1))

    level = one(*cuts[0])
    for cut in cuts[1:]:
        level = level * one(*cut)
    return level


def bell_draw(stream_key, extent, width, reach, pieces=(), kind=jnp.bfloat16):
    level = level_of(stream_key, extent, pieces, -0.22, 0.18) if pieces else 1.0
    array = jax.random.normal(stream_key, extent, jnp.float32) * width * level
    return jnp.minimum(jnp.maximum(array, -reach), reach).astype(kind)


def heavy_noise(own_key, extent, width, bound, shards, heavy, held_as=jnp.bfloat16):
    drawn = width * jax.random.normal(own_key, extent, jnp.float32)
    if shards:
        drawn = drawn * level_of(own_key, extent, shards, -0.22, 0.18)
    return jnp.clip(spiked(drawn, jax.random.fold_in(own_key, 3), *heavy), -bound, bound).astype(held_as)


def setup_inputs(seed: int = 0, part: int = 0) -> dict:
    arg_keys = jax.random.split(jax.random.key(seed), 10)
    part_splits = jax.random.split(jax.random.fold_in(arg_keys[9], part), 10)
    residual = draw_residual(jax.random.fold_in(jax.random.fold_in(arg_keys[9], part), 71), part)
    gain_first = jnp.clip(1.0 + 0.18 * jax.random.normal(arg_keys[1], (D,), jnp.float32), 0.099609375, 1.8984375).astype(jnp.bfloat16)
    gate_first = bell_draw(arg_keys[2], (D, FF), D ** -0.5, 0.09375, ((0, 16), (1, 16)))
    up_first = bell_draw(arg_keys[3], (D, FF), D ** -0.5, 0.09375, ((0, 16), (1, 16)))
    down_first = heavy_noise(arg_keys[4], (FF, D), FF ** -0.5, 0.078125, ((0, 16), (1, 16)), (0, 1, 16, 2.0))
    gain_second = jnp.clip(1.0 + 0.18 * jax.random.normal(arg_keys[5], (D,), jnp.float32), 0.099609375, 1.8984375).astype(jnp.bfloat16)
    gate_second = bell_draw(arg_keys[6], (D, FF), D ** -0.5, 0.09375, ((0, 16), (1, 16)))
    up_second = bell_draw(arg_keys[7], (D, FF), D ** -0.5, 0.09375, ((0, 16), (1, 16)))
    down_second = heavy_noise(arg_keys[8], (FF, D), FF ** -0.5, 0.078125, ((0, 16), (1, 16)), (0, 1, 16, 2.0))
    return dict(residual=residual, gain_first=gain_first, gate_first=gate_first, up_first=up_first, down_first=down_first, gain_second=gain_second, gate_second=gate_second, up_second=up_second, down_second=down_second)


epsilon = 1e-06

def half_step(stream, gain, w_gate, w_up, w_down):
    values = stream.astype(jnp.float32)
    scale = lax.rsqrt(lax.optimization_barrier(jnp.mean(values * values, axis=1, keepdims=True)) + epsilon)
    normed = (values * gain.astype(jnp.float32)).astype(jnp.bfloat16)
    gate = scale * jnp.dot(normed, w_gate, preferred_element_type=jnp.float32)
    upward = scale * jnp.dot(normed, w_up, preferred_element_type=jnp.float32)
    hidden = (jax.nn.silu(gate) * upward).astype(jnp.bfloat16)
    branch = jnp.dot(hidden, w_down, preferred_element_type=jnp.float32)
    return (values + 0.5 * branch).astype(jnp.bfloat16)

def reference(residual, gain_first, gate_first, up_first, down_first, gain_second, gate_second, up_second, down_second):
    middle = half_step(residual, gain_first, gate_first, up_first, down_first)
    return half_step(middle, gain_second, gate_second, up_second, down_second)
```

```python
import jax
import jax.numpy as jnp
from jax import lax
from jax.sharding import PartitionSpec as P

LANES = 128

epsilon = 1e-06


def exchanged(array, axis):
    return lax.all_to_all(array, axis, 0, 0, tiled=True)


def sent_to_all(array, axis):
    peers = lax.axis_size(axis)
    return exchanged(jnp.broadcast_to(array[None], (peers, *array.shape)), axis)


def in_two_halves(value):
    high = value.astype(jnp.bfloat16)
    low = (value - high.astype(jnp.float32)).astype(jnp.bfloat16)
    return high, low


def half_step(stream, gain, w_gate, w_up, w_down):
    width = stream.shape[1] * lax.axis_size("ra")
    tokens = stream.shape[0]
    units = w_gate.shape[1]
    ra, cb = lax.axis_size("ra"), lax.axis_size("cb")
    values = stream.astype(jnp.float32)
    square_part = jnp.sum(values * values, axis=1, keepdims=True)
    normed = (values * gain.astype(jnp.float32)).astype(jnp.bfloat16)
    gate_part = jnp.dot(normed, w_gate, preferred_element_type=jnp.float32)
    up_part = jnp.dot(normed, w_up, preferred_element_type=jnp.float32)
    high, low = in_two_halves(square_part)
    squares = jnp.concatenate([high, low, jnp.zeros((tokens, LANES - 2), jnp.bfloat16)], axis=1)
    parts = jnp.concatenate(
        [gate_part.astype(jnp.bfloat16), up_part.astype(jnp.bfloat16), squares], axis=1
    )
    parts = exchanged(parts.reshape(ra, tokens // ra, parts.shape[1]), "ra")
    total = jnp.sum(parts.astype(jnp.float32), axis=0)
    gate_sum, up_sum = total[:, :units], total[:, units : 2 * units]
    square_sum = total[:, 2 * units : 2 * units + 1] + total[:, 2 * units + 1 : 2 * units + 2]
    scale = lax.rsqrt(square_sum / width + epsilon)
    hidden = (jax.nn.silu(scale * gate_sum) * (scale * up_sum)).astype(jnp.bfloat16)
    hidden = sent_to_all(hidden, "ra").reshape(tokens, units)
    down_part = jnp.dot(hidden, w_down, preferred_element_type=jnp.float32)
    pieces = exchanged(
        down_part.astype(jnp.bfloat16).reshape(cb, tokens // cb, stream.shape[1]), "cb"
    )
    branch = jnp.sum(pieces.astype(jnp.float32), axis=0)
    own = lax.dynamic_slice_in_dim(
        stream, lax.axis_index("cb") * (tokens // cb), tokens // cb, axis=0
    )
    updated = (own.astype(jnp.float32) + 0.5 * branch).astype(jnp.bfloat16)
    return sent_to_all(updated, "cb").reshape(stream.shape)


def per_device(
    residual,
    gain_first,
    gate_first,
    up_first,
    down_first,
    gain_second,
    gate_second,
    up_second,
    down_second,
):
    middle = half_step(residual, gain_first, gate_first, up_first, down_first)
    return half_step(middle, gain_second, gate_second, up_second, down_second)


def solution(mesh):
    in_specs = (
        P("grp", "ra"),
        P("ra"),
        P("ra", "cb"),
        P("ra", "cb"),
        P("cb", "ra"),
        P("ra"),
        P("ra", "cb"),
        P("ra", "cb"),
        P("cb", "ra"),
    )
    out_specs = P("grp", "ra")
    return jax.shard_map(
        per_device, mesh=mesh, in_specs=in_specs, out_specs=out_specs, check_vma=False
    )
```
